32 devices in a mesh: sp: 8 (over z, x), tp: 4 (over y, core).
Axes of the slice: x: 2, y: 2, z: 4, core: 2. Of those that a mesh axis runs over, the one named last changes fastest.
Arguments:
- stratum_source_matrix: bfloat16 [1024, 2048], P('sp'), may hold values from -70 to 70
- acceptance_query: bfloat16 [2, 1024, 1024], P(None, 'sp', 'tp'), may hold values from -6 to 6
- cluster_lookup_matrix: bfloat16 [2, 1024, 1024], P(None, 'sp', 'tp'), may hold values from -6 to 6
- cluster_payload_matrix: bfloat16 [2, 1024, 1024], P(None, 'sp', 'tp'), may hold values from -6 to 6
- fading_logit: bfloat16 [2, 1024, 1024], P(None, 'sp', 'tp'), may hold values from -17 to 2
- adaptation_speed_logit: bfloat16 [2, 1024, 1024], P(None, 'sp', 'tp'), may hold values from -14 to 5
- additional_fading_exponent: float32 [2, 1024, 1024], P(None, 'sp', 'tp'), may hold values from -0.7 to 0
- result_switch_pair: bfloat16 [2, 1024, 1024], P(None, 'sp', 'tp'), may hold values from -6 to 6
- attender_scaling_factor: float32 [2, 1024], P(None, 'tp'), may hold values from 0.1 to 1.9
- present_item_factor: float32 [2, 1024], P(None, 'tp'), may hold values from -0.9 to 0.9
- final_mapping_matrix: bfloat16 [2, 1024, 2048], P(None, 'tp'), may hold values from -0.125 to 0.125
- perceptron_scaling_factor: float32 [2048], replicated, may hold values from 0.1 to 1.9
- switching_matrix: bfloat16 [2048, 5632], P('sp', 'tp'), may hold values from -0.125 to 0.125
- widening_matrix: bfloat16 [2048, 5632], P('sp', 'tp'), may hold values from -0.125 to 0.125
- shrinking_matrix: bfloat16 [5632, 2048], P('tp', 'sp'), may hold values from -0.078125 to 0.078125
Outputs:
- layer_out: bfloat16 [1024, 2048], P('sp', 'tp')
The draws below stay inside these ranges and needn't reach their ends.
All inputs are finite; a program needn't handle non-finite values.
Results may differ from the reference program's by a relative error of at most 0.014.
Values may be sent and summed in bfloat16 or wider, within the bound.
A program may use at most 128 MiB of HBM per device.

```python
import math
import jax
import jax.numpy as jnp
from jax import lax

D = 2048
FF = 5632
CLUSTER_FEATURES = 1024
DS = 64
DL = 128
TOK_DEV = 128
SEQUENCE_TOKENS = 1024
N_TP = 4


def fast_heads(key):
    fast_share = 0.5
    small_heads = jax.random.uniform(jax.random.fold_in(key, 101), (CLUSTER_FEATURES // DS,)) < fast_share
    large_heads = jax.random.uniform(jax.random.fold_in(key, 102), (CLUSTER_FEATURES // DL,)) < fast_share
    return jnp.stack([jnp.repeat(small_heads, DS), jnp.repeat(large_heads, DL)])


def rough_entries(key):
    return jnp.clip(jax.random.normal(key, (2, SEQUENCE_TOKENS, CLUSTER_FEATURES)), -4.0, 4.0)


def draw_fading_logit(key, part):
    fast_mask = fast_heads(key)
    level = jnp.where(fast_mask, -3.5, -12.0)
    jitter = rough_entries(jax.random.fold_in(key, 201))
    block_shift = jax.random.uniform(jax.random.fold_in(key, 202), (2, SEQUENCE_TOKENS // TOK_DEV, 1), minval=-0.7, maxval=0.7)
    block_shift = jnp.repeat(block_shift, TOK_DEV, axis=1)
    return (level[:, None, :] + jitter + block_shift).astype(jnp.bfloat16)


def draw_adaptation_speed_logit(key, part):
    fast_mask = fast_heads(key)
    slow_small = math.log(0.4 * DS / SEQUENCE_TOKENS)
    slow_large = math.log(0.4 * DL / SEQUENCE_TOKENS)
    slow_level = jnp.stack([jnp.full((CLUSTER_FEATURES,), slow_small, jnp.float32), jnp.full((CLUSTER_FEATURES,), slow_large, jnp.float32)])
    level = jnp.where(fast_mask, 0.0, slow_level)
    jitter = rough_entries(jax.random.fold_in(key, 301))
    return (level[:, None, :] + jitter).astype(jnp.float32).astype(jnp.bfloat16)


def draw_additional_fading_exponent(key, part):
    extra_decay_rows = jax.random.randint(jax.random.fold_in(key, 401), (2, 3), 0, SEQUENCE_TOKENS)
    sequence_positions = jnp.arange(SEQUENCE_TOKENS)
    corrected_state = jnp.any(sequence_positions[None, :, None] == extra_decay_rows[:, None, :], axis=-1)
    extra_decay_depth = jax.random.uniform(jax.random.fold_in(key, 402), (2, SEQUENCE_TOKENS, CLUSTER_FEATURES), minval=math.log(0.5), maxval=math.log(0.8))
    return jnp.where(corrected_state[:, :, None], extra_decay_depth, 0.0).astype(jnp.float32)


def draw_stratum_source_matrix(key, part):
    spread = jnp.arange(D).astype(jnp.float32) / D
    column_scale = 0.5 * 3.0 ** spread * jnp.exp(jax.random.uniform(jax.random.fold_in(key, 501), (D,), minval=-0.6, maxval=0.6))
    row_scale = jnp.exp(jax.random.uniform(jax.random.fold_in(key, 502), (SEQUENCE_TOKENS, 1), minval=math.log(0.4), maxval=math.log(4.0)))
    entries = jnp.clip(jax.random.normal(jax.random.fold_in(key, 503), (SEQUENCE_TOKENS, D)), -6.0, 6.0)
    return (entries * row_scale * column_scale).astype(jnp.float32).astype(jnp.bfloat16)


def levels(own_key, extent, shards, smallest, top_value):
    factor_of = 1.0
    for axis_at, shards_of in shards:
        steps = jax.random.uniform(jax.random.fold_in(jax.random.fold_in(own_key, 6), axis_at), (shards_of,), jnp.float32, smallest / len(shards), top_value / len(shards))
        factor_of = factor_of * jnp.repeat(jnp.exp(steps), extent[axis_at] // shards_of).reshape((-1,) + (1,) * (len(extent) - 1 - axis_at))
    return factor_of


def scatter_about(own_key, dims, width, bound, shards=(), kind=jnp.bfloat16):
    loudness = levels(own_key, dims, shards, -0.22, 0.18) if shards else 1.0
    array = jax.random.normal(own_key, dims, jnp.float32) * width * loudness
    return jnp.minimum(jnp.maximum(array, -bound), bound).astype(kind)


def setup_inputs(seed: int = 0) -> dict:
    arg_keys = jax.random.split(jax.random.key(seed), 16)
    return {
        "stratum_source_matrix": draw_stratum_source_matrix(jax.random.fold_in(arg_keys[15], 71), 0),
        "acceptance_query": scatter_about(arg_keys[1], (2, SEQUENCE_TOKENS, CLUSTER_FEATURES), 1.0, 6.0, ((1, 8), (2, 4))),
        "cluster_lookup_matrix": scatter_about(arg_keys[2], (2, SEQUENCE_TOKENS, CLUSTER_FEATURES), 1.0, 6.0, ((1, 8), (2, 4))),
        "cluster_payload_matrix": scatter_about(arg_keys[3], (2, SEQUENCE_TOKENS, CLUSTER_FEATURES), 1.0, 6.0, ((1, 8), (2, 4))),
        "fading_logit": draw_fading_logit(jax.random.fold_in(arg_keys[15], 71), 0),
        "adaptation_speed_logit": draw_adaptation_speed_logit(jax.random.fold_in(arg_keys[15], 71), 0),
        "additional_fading_exponent": draw_additional_fading_exponent(jax.random.fold_in(arg_keys[15], 71), 0),
        "result_switch_pair": scatter_about(arg_keys[7], (2, SEQUENCE_TOKENS, CLUSTER_FEATURES), 1.0, 6.0, ((1, 8), (2, 4))),
        "attender_scaling_factor": jnp.clip(1.0 + 0.18 * jax.random.normal(arg_keys[8], (2, CLUSTER_FEATURES), jnp.float32), 0.1, 1.9),
        "present_item_factor": scatter_about(arg_keys[9], (2, CLUSTER_FEATURES), 0.15, 0.9, ((1, 4),), jnp.float32),
        "final_mapping_matrix": scatter_about(arg_keys[10], (2, CLUSTER_FEATURES, D), (2 * CLUSTER_FEATURES) ** -0.5, 0.125, ((1, 4),)),
        "perceptron_scaling_factor": jnp.clip(1.0 + 0.18 * jax.random.normal(arg_keys[11], (D,), jnp.float32), 0.1, 1.9),
        "switching_matrix": scatter_about(arg_keys[12], (D, FF), D ** -0.5, 0.125, ((0, 8), (1, 4))),
        "widening_matrix": scatter_about(arg_keys[13], (D, FF), D ** -0.5, 0.125, ((0, 8), (1, 4))),
        "shrinking_matrix": scatter_about(arg_keys[14], (FF, D), FF ** -0.5, 0.078125, ((0, 4), (1, 8))),
    }


highest = lax.Precision.HIGHEST
norm_epsilon = 1e-06
head_epsilon = 0.00064
key_epsilon = 1e-06

def per_head_terms(acceptance_query, cluster_lookup_matrix, cluster_payload_matrix, fading_logit, adaptation_speed_logit, additional_fading_exponent, attender_feature_count):
    row_count, channels = acceptance_query.shape
    lattice_layout = (row_count, channels // attender_feature_count, attender_feature_count)
    acceptance_lines = acceptance_query.astype(jnp.float32).reshape(lattice_layout)
    mapped_lookups = cluster_lookup_matrix.astype(jnp.float32).reshape(lattice_layout)
    mapped_payloads = cluster_payload_matrix.astype(jnp.float32).reshape(lattice_layout)
    learning_rate_logarithm = -jax.nn.softplus(-fading_logit.astype(jnp.float32)) - 0.5
    decay_logarithm = (additional_fading_exponent - jnp.exp(learning_rate_logarithm)).reshape(lattice_layout)
    learn_rate = jax.nn.sigmoid(adaptation_speed_logit.astype(jnp.float32)).reshape(lattice_layout)
    removal = mapped_lookups * lax.rsqrt(lax.optimization_barrier(jnp.sum(mapped_lookups * mapped_lookups, axis=-1, keepdims=True)) + key_epsilon)
    return (acceptance_lines, mapped_lookups, mapped_payloads, decay_logarithm, -removal, learn_rate * removal)

def entire_cluster(raw_retrieval, acceptance_lines, mapped_lookups, mapped_payloads, scaling_array, diagonal_reward_array, switch_amounts):
    row_count, attender_count, attender_feature_count = raw_retrieval.shape
    row_mean = lax.optimization_barrier(jnp.mean(raw_retrieval, axis=-1, keepdims=True))
    centered = raw_retrieval - row_mean
    variance = lax.optimization_barrier(jnp.mean(centered * centered, axis=-1, keepdims=True))
    normed = centered * lax.rsqrt(variance + head_epsilon) * scaling_array.reshape(attender_count, attender_feature_count)
    diagonal_item_contribution = lax.optimization_barrier(jnp.sum(acceptance_lines * mapped_lookups * diagonal_reward_array.reshape(attender_count, attender_feature_count), axis=-1, keepdims=True)) * mapped_payloads
    joined = (normed + diagonal_item_contribution).reshape(row_count, attender_count * attender_feature_count)
    return (joined * switch_amounts.astype(jnp.float32)).astype(jnp.bfloat16)

def advance_one(memory, acceptance_lines, mapped_lookups, mapped_payloads, decay_logarithm, remove_left, remove_right):
    removed = jnp.einsum('hij,hj->hi', memory, remove_left, precision=highest)
    memory = memory * jnp.exp(decay_logarithm)[:, None, :] + removed[:, :, None] * remove_right[:, None, :] + mapped_payloads[:, :, None] * mapped_lookups[:, None, :]
    return (memory, jnp.einsum('hij,hj->hi', memory, acceptance_lines, precision=highest))

def recurrence(terms_small, terms_large):

    def advance(memories, inputs):
        memory_small, read_small = advance_one(memories[0], *inputs[0])
        memory_large, read_large = advance_one(memories[1], *inputs[1])
        return ((memory_small, memory_large), (read_small, read_large))
    initial = tuple((jnp.zeros((aggregated_contributions[0].shape[1], aggregated_contributions[0].shape[2], aggregated_contributions[0].shape[2]), jnp.float32) for aggregated_contributions in (terms_small, terms_large)))
    final_memories, retrieved_result_lines = lax.scan(advance, initial, (terms_small, terms_large))
    return retrieved_result_lines

def reference(stratum_source_matrix, acceptance_query, cluster_lookup_matrix, cluster_payload_matrix, fading_logit, adaptation_speed_logit, additional_fading_exponent, result_switch_pair, attender_scaling_factor, present_item_factor, final_mapping_matrix, perceptron_scaling_factor, switching_matrix, widening_matrix, shrinking_matrix):
    group_widths = (DS, DL)
    aggregated_contributions = [per_head_terms(acceptance_query[cluster_ordinal], cluster_lookup_matrix[cluster_ordinal], cluster_payload_matrix[cluster_ordinal], fading_logit[cluster_ordinal], adaptation_speed_logit[cluster_ordinal], additional_fading_exponent[cluster_ordinal], group_widths[cluster_ordinal]) for cluster_ordinal in range(2)]
    retrieved_result_lines = recurrence(tuple(aggregated_contributions[0]), tuple(aggregated_contributions[1]))
    blended_result = [entire_cluster(retrieved_result_lines[cluster_ordinal], aggregated_contributions[cluster_ordinal][0], aggregated_contributions[cluster_ordinal][1], aggregated_contributions[cluster_ordinal][2], attender_scaling_factor[cluster_ordinal], present_item_factor[cluster_ordinal], result_switch_pair[cluster_ordinal]) for cluster_ordinal in range(2)]
    slice_width = CLUSTER_FEATURES // N_TP
    branch = jnp.zeros((SEQUENCE_TOKENS, D), jnp.float32)
    for slice_index in range(N_TP):
        lower = slice_index * slice_width
        upper = lower + slice_width
        partial_value = jnp.dot(blended_result[0][:, lower:upper], final_mapping_matrix[0, lower:upper], preferred_element_type=jnp.float32) + jnp.dot(blended_result[1][:, lower:upper], final_mapping_matrix[1, lower:upper], preferred_element_type=jnp.float32)
        branch = branch + lax.optimization_barrier(partial_value.astype(jnp.bfloat16)).astype(jnp.float32)
    hidden_state = (stratum_source_matrix.astype(jnp.float32) + branch).astype(jnp.bfloat16)
    state_float = hidden_state.astype(jnp.float32)
    mean_square = lax.optimization_barrier(jnp.mean(state_float * state_float, axis=1, keepdims=True))
    normed = (state_float * lax.rsqrt(mean_square + norm_epsilon) * perceptron_scaling_factor).astype(jnp.bfloat16)
    gate_pre = jnp.dot(normed, switching_matrix, preferred_element_type=jnp.float32)
    up_pre = jnp.dot(normed, widening_matrix, preferred_element_type=jnp.float32)
    activated = (jax.nn.silu(gate_pre) * up_pre).astype(jnp.bfloat16)
    hidden_width = FF // N_TP
    mixer = jnp.zeros((SEQUENCE_TOKENS, D), jnp.float32)
    for slice_index in range(N_TP):
        lower = slice_index * hidden_width
        upper = lower + hidden_width
        partial_value = jnp.dot(activated[:, lower:upper], shrinking_matrix[lower:upper], preferred_element_type=jnp.float32)
        mixer = mixer + lax.optimization_barrier(partial_value.astype(jnp.bfloat16)).astype(jnp.float32)
    return (state_float + mixer).astype(jnp.bfloat16)
```

```python
import functools

import jax
import jax.numpy as jnp
from jax import lax
from jax.experimental import pallas as pl
from jax.experimental.pallas import tpu as pltpu
from jax.sharding import PartitionSpec as P

DS = 64
DL = 128
LANES = 128
MESH = pl.DeviceIdType.MESH

norm_epsilon = 1e-06
head_epsilon = 0.00064
key_epsilon = 1e-06


NN = (((1,), (0,)), ((), ()))
NT = (((1,), (1,)), ((), ()))


def split(x, count=2):
    if x.dtype == jnp.bfloat16:
        return [x]
    parts = []
    for _ in range(count - 1):
        high = x.astype(jnp.bfloat16)
        parts.append(high)
        x = x - high.astype(jnp.float32)
    return parts + [x.astype(jnp.bfloat16)]


def product(a, b, dims, count=2):
    total = None
    for i, p in enumerate(split(a, count)):
        for j, r in enumerate(split(b, count)):
            if i + j < count:
                term = lax.dot_general(p, r, dims, preferred_element_type=jnp.float32)
                total = term if total is None else total + term
    return total


def mm(a, b, count=2):
    return product(a, b, NN, count)


def mm_nt(a, b):
    return product(a, b, NT)


def sigmoid(x):
    return 1.0 / (1.0 + jnp.exp(-x))


def same_head(width):
    i = lax.broadcasted_iota(jnp.int32, (LANES, LANES), 0) // width
    j = lax.broadcasted_iota(jnp.int32, (LANES, LANES), 1) // width
    return (i == j).astype(jnp.float32).astype(jnp.bfloat16)


def unit_inverse(strict_part, rows, cols):
    size = strict_part.shape[0]
    inverse = (rows == cols).astype(jnp.float32)
    half = 1
    while half < size:
        off = (rows // (2 * half) == cols // (2 * half)) & (rows // half != cols // half)
        part = jnp.where(off, strict_part, 0.0)
        if half == 1:
            inverse = inverse + part
        else:
            inverse = inverse + mm(mm(inverse, part), inverse)
        half *= 2
    return inverse


def local_unit(width, q, k, v, fade, speed, extra):
    T = q.shape[0]
    ones = same_head(width)
    log_decay = extra - jnp.exp(jnp.float32(-0.5)) * sigmoid(fade)
    removal = k * lax.rsqrt(mm(k * k, ones) + key_epsilon)
    left = -removal
    right = sigmoid(speed) * removal
    rows = lax.broadcasted_iota(jnp.int32, (T, T), 0)
    cols = lax.broadcasted_iota(jnp.int32, (T, T), 1)
    inclusive = rows >= cols
    strict = rows > cols
    cumulative = mm(inclusive.astype(jnp.float32).astype(jnp.bfloat16), log_decay, 3)
    middle = cumulative[T // 2 : T // 2 + 1, :]
    final = cumulative[T - 1 : T, :]
    forward = jnp.exp(cumulative - middle)
    backward = jnp.exp(middle - cumulative)
    tail = jnp.exp(final - cumulative)
    queries = jnp.concatenate([left * jnp.exp(-log_decay) * forward, q * forward], axis=0)
    sources = jnp.concatenate([right * backward, k * backward], axis=0)
    start_target = left * jnp.exp(cumulative - log_decay)
    right_tail = right * tail
    key_tail = k * tail
    eye = lax.broadcasted_iota(jnp.int32, (LANES, LANES), 0) == lax.broadcasted_iota(
        jnp.int32, (LANES, LANES), 1
    )
    transit = jnp.where(eye, jnp.exp(final), 0.0)
    start_read = q * jnp.exp(cumulative)
    added = jnp.zeros((LANES, LANES), jnp.float32)
    local_out = jnp.zeros((T, LANES), jnp.float32)
    lane = lax.broadcasted_iota(jnp.int32, (1, LANES), 1) // width
    for head in range(LANES // width):
        only = lane == head
        pick = (lambda a: a) if width == LANES else (lambda a: jnp.where(only, a, 0.0))
        pairs = mm_nt(pick(queries), sources)
        remove_remove = jnp.where(strict, pairs[:T, :T], 0.0)
        remove_key = jnp.where(strict, pairs[:T, T:], 0.0)
        read_remove = jnp.where(inclusive, pairs[T:, :T], 0.0)
        read_key = jnp.where(inclusive, pairs[T:, T:], 0.0)
        inverse = unit_inverse(remove_remove, rows, cols)
        value = pick(v)
        carried = mm(inverse, mm(remove_key, value))
        start = mm(inverse, pick(start_target))
        local_out = local_out + mm(read_remove, carried) + mm(read_key, value)
        start_read = start_read + mm(read_remove, start)
        head_right = pick(right_tail)
        transit = transit + mm(start.T, head_right)
        added = added + mm(carried.T, head_right) + mm(value.T, pick(key_tail))
    return local_out, start_read, transit, added


def finish_unit(width, read, q, k, v, gain, own, gate):
    ones = same_head(width)
    mean = mm(read, ones) / width
    centered = read - mean
    variance = mm(centered * centered, ones) / width
    normed = centered * lax.rsqrt(variance + head_epsilon) * gain
    diagonal = mm(q * k * own, ones) * v
    return ((normed + diagonal) * gate).astype(jnp.bfloat16)


def attention_kernel(
    n_sp, widths, q_ref, k_ref, v_ref, f_ref, a_ref, e_ref, g_ref, gain_ref, own_ref,
    mixed_ref, local_ref, read_ref, mine, got, send_sem, recv_sem,
):
    me = lax.axis_index("sp")
    tp = lax.axis_index("tp")

    barrier = pltpu.get_barrier_semaphore()

    @pl.loop(1, n_sp)
    def _(d):
        pl.semaphore_signal(
            barrier, inc=1, device_id=(lax.rem(me + d, n_sp), tp), device_id_type=MESH
        )

    pl.semaphore_wait(barrier, n_sp - 1)

    per_group = q_ref.shape[2] // LANES

    def load(ref, g, c):
        return ref[g, :, c * LANES : (c + 1) * LANES].astype(jnp.float32)

    def copy(u, d, to):
        return pltpu.make_async_remote_copy(
            src_ref=mine.at[u],
            dst_ref=got.at[d, u],
            send_sem=send_sem.at[u, d],
            recv_sem=recv_sem.at[u, d],
            device_id=(to, tp),
            device_id_type=MESH,
        )

    units = [(g, c) for g in range(2) for c in range(per_group)]
    for u, (g, c) in enumerate(units):
        local_out, start_read, transit, added = local_unit(
            widths[g], *(load(r, g, c) for r in (q_ref, k_ref, v_ref, f_ref, a_ref, e_ref))
        )
        local_ref[u] = local_out
        read_ref[u] = start_read
        mine[u, 0] = transit.astype(jnp.bfloat16)
        mine[u, 1] = added.astype(jnp.bfloat16)

        @pl.loop(1, n_sp)
        def _(d):
            @pl.when(me + d < n_sp)
            def _():
                copy(u, d, me + d).start()

    for u in range(len(units)):

        @pl.loop(1, n_sp)
        def _(d):
            @pl.when(me - d >= 0)
            def _():
                copy(u, d, me).wait_recv()

    def fold(step, states):
        d = me - step
        return tuple(
            mm(s, got[d, u, 0]) + got[d, u, 1].astype(jnp.float32)
            for u, s in enumerate(states)
        )

    states = lax.fori_loop(
        0, me, fold, tuple(jnp.zeros((LANES, LANES), jnp.float32) for _ in units)
    )
    for u, (g, c) in enumerate(units):
        lanes = slice(c * LANES, (c + 1) * LANES)
        read = local_ref[u] + mm_nt(read_ref[u], states[u])
        mixed = finish_unit(
            widths[g], read, load(q_ref, g, c), load(k_ref, g, c), load(v_ref, g, c),
            gain_ref[g : g + 1, lanes], own_ref[g : g + 1, lanes], load(g_ref, g, c),
        )
        mixed_ref[:, u * LANES : (u + 1) * LANES] = mixed

    for u in range(len(units)):

        @pl.loop(1, n_sp)
        def _(d):
            @pl.when(me + d < n_sp)
            def _():
                copy(u, d, me + d).wait_send()


def attention(n_sp, q, k, v, f, a, e, g, gain, own):
    T, channels = q.shape[1], q.shape[2]
    units = 2 * channels // LANES
    vmem = pl.BlockSpec(memory_space=pltpu.VMEM)
    return pl.pallas_call(
        functools.partial(attention_kernel, n_sp, (DS, DL)),
        out_shape=jax.ShapeDtypeStruct((T, 2 * channels), jnp.bfloat16),
        in_specs=[vmem] * 9,
        out_specs=vmem,
        scratch_shapes=[
            pltpu.VMEM((units, T, LANES), jnp.float32),
            pltpu.VMEM((units, T, LANES), jnp.float32),
            pltpu.VMEM((units, 2, LANES, LANES), jnp.bfloat16),
            pltpu.VMEM((n_sp, units, 2, LANES, LANES), jnp.bfloat16),
            pltpu.SemaphoreType.DMA((units, n_sp)),
            pltpu.SemaphoreType.DMA((units, n_sp)),
        ],
        compiler_params=pltpu.CompilerParams(
            collective_id=0, has_side_effects=True, vmem_limit_bytes=40 * 2**20
        ),
        cost_estimate=pl.CostEstimate(
            flops=4 * 10**8, bytes_accessed=2**21, transcendentals=0
        ),
        name="attention",
    )(q, k, v, f, a, e, g, gain, own)


def on_device(
    stratum_source_matrix,
    acceptance_query,
    cluster_lookup_matrix,
    cluster_payload_matrix,
    fading_logit,
    adaptation_speed_logit,
    additional_fading_exponent,
    result_switch_pair,
    attender_scaling_factor,
    present_item_factor,
    final_mapping_matrix,
    perceptron_scaling_factor,
    switching_matrix,
    widening_matrix,
    shrinking_matrix,
):
    gate_whole, up_whole = (
        lax.all_gather(switching_matrix, "sp", axis=0, tiled=True),
        lax.all_gather(widening_matrix, "sp", axis=0, tiled=True),
    )
    mixed = attention(
        lax.axis_size("sp"),
        acceptance_query,
        cluster_lookup_matrix,
        cluster_payload_matrix,
        fading_logit,
        adaptation_speed_logit,
        additional_fading_exponent,
        result_switch_pair,
        attender_scaling_factor,
        present_item_factor,
    )
    partial_value = jnp.dot(
        mixed,
        final_mapping_matrix.reshape(-1, final_mapping_matrix.shape[2]),
        preferred_element_type=jnp.float32,
    )
    columns = perceptron_scaling_factor.shape[0] // lax.axis_size("tp")
    own_start = lax.axis_index("tp") * columns
    residual_float = stratum_source_matrix.astype(jnp.float32)
    branch = lax.psum_scatter(
        partial_value.astype(jnp.bfloat16), "tp", scatter_dimension=1, tiled=True
    ).astype(jnp.float32)
    own_residual = lax.dynamic_slice_in_dim(residual_float, own_start, columns, 1)
    own_state = (own_residual + branch).astype(jnp.bfloat16).astype(jnp.float32)
    square_total = lax.psum(jnp.sum(own_state * own_state, axis=1), "tp")
    own_gain = lax.dynamic_slice_in_dim(perceptron_scaling_factor, own_start, columns, 0)
    scaled = (
        own_state
        * lax.rsqrt(square_total / perceptron_scaling_factor.shape[0] + norm_epsilon)[:, None]
        * own_gain
    )
    normed = lax.all_gather(scaled.astype(jnp.bfloat16), "tp", axis=1, tiled=True)
    gate_pre = jnp.dot(normed, gate_whole, preferred_element_type=jnp.float32)
    up_pre = jnp.dot(normed, up_whole, preferred_element_type=jnp.float32)
    activated = (jax.nn.silu(gate_pre) * up_pre).astype(jnp.bfloat16)
    down_terms = jnp.dot(
        activated,
        lax.all_gather(shrinking_matrix, "sp", axis=1, tiled=True),
        preferred_element_type=jnp.float32,
    )
    mixer = lax.psum_scatter(
        down_terms.astype(jnp.bfloat16), "tp", scatter_dimension=1, tiled=True
    ).astype(jnp.float32)
    return (own_state + mixer).astype(jnp.bfloat16)


def solution(mesh):
    tokens = P(None, "sp", "tp")
    in_specs = (
        P("sp", None), tokens, tokens, tokens, tokens, tokens, tokens, tokens,
        P(None, "tp"), P(None, "tp"), P(None, "tp", None), P(),
        P("sp", "tp"), P("sp", "tp"), P("tp", "sp"),
    )
    return jax.shard_map(
        on_device, mesh=mesh, in_specs=in_specs, out_specs=P("sp", "tp"), check_vma=False
    )
```

```python
import functools

import jax
import jax.numpy as jnp
from jax import lax
from jax.experimental import pallas as pl
from jax.experimental.pallas import tpu as pltpu
from jax.sharding import PartitionSpec as P

DS = 64
DL = 128
LANES = 128
MESH = pl.DeviceIdType.MESH

norm_epsilon = 1e-06
head_epsilon = 0.00064
key_epsilon = 1e-06


NN = (((1,), (0,)), ((), ()))
NT = (((1,), (1,)), ((), ()))


def split(x, count=2):
    if x.dtype == jnp.bfloat16:
        return [x]
    parts = []
    for _ in range(count - 1):
        high = x.astype(jnp.bfloat16)
        parts.append(high)
        x = x - high.astype(jnp.float32)
    return parts + [x.astype(jnp.bfloat16)]


def product(a, b, dims, count=2):
    total = None
    for i, p in enumerate(split(a, count)):
        for j, r in enumerate(split(b, count)):
            if i + j < count:
                term = lax.dot_general(p, r, dims, preferred_element_type=jnp.float32)
                total = term if total is None else total + term
    return total


def mm(a, b, count=2):
    return product(a, b, NN, count)


def mm_nt(a, b):
    return product(a, b, NT)


def sigmoid(x):
    return 1.0 / (1.0 + jnp.exp(-x))


def same_head(width):
    i = lax.broadcasted_iota(jnp.int32, (LANES, LANES), 0) // width
    j = lax.broadcasted_iota(jnp.int32, (LANES, LANES), 1) // width
    return (i == j).astype(jnp.float32).astype(jnp.bfloat16)


def unit_inverse(strict_part, rows, cols):
    size = strict_part.shape[0]
    inverse = (rows == cols).astype(jnp.float32)
    half = 1
    while half < size:
        off = (rows // (2 * half) == cols // (2 * half)) & (rows // half != cols // half)
        part = jnp.where(off, strict_part, 0.0)
        if half == 1:
            inverse = inverse + part
        else:
            inverse = inverse + mm(mm(inverse, part), inverse)
        half *= 2
    return inverse


def local_unit(width, q, k, v, fade, speed, extra):
    T = q.shape[0]
    ones = same_head(width)
    log_decay = extra - jnp.exp(jnp.float32(-0.5)) * sigmoid(fade)
    removal = k * lax.rsqrt(mm(k * k, ones) + key_epsilon)
    left = -removal
    right = sigmoid(speed) * removal
    rows = lax.broadcasted_iota(jnp.int32, (T, T), 0)
    cols = lax.broadcasted_iota(jnp.int32, (T, T), 1)
    inclusive = rows >= cols
    strict = rows > cols
    cumulative = mm(inclusive.astype(jnp.float32).astype(jnp.bfloat16), log_decay, 3)
    middle = cumulative[T // 2 : T // 2 + 1, :]
    final = cumulative[T - 1 : T, :]
    forward = jnp.exp(cumulative - middle)
    backward = jnp.exp(middle - cumulative)
    tail = jnp.exp(final - cumulative)
    queries = jnp.concatenate([left * jnp.exp(-log_decay) * forward, q * forward], axis=0)
    sources = jnp.concatenate([right * backward, k * backward], axis=0)
    start_target = left * jnp.exp(cumulative - log_decay)
    right_tail = right * tail
    key_tail = k * tail
    eye = lax.broadcasted_iota(jnp.int32, (LANES, LANES), 0) == lax.broadcasted_iota(
        jnp.int32, (LANES, LANES), 1
    )
    transit = jnp.where(eye, jnp.exp(final), 0.0)
    start_read = q * jnp.exp(cumulative)
    added = jnp.zeros((LANES, LANES), jnp.float32)
    local_out = jnp.zeros((T, LANES), jnp.float32)
    lane = lax.broadcasted_iota(jnp.int32, (1, LANES), 1) // width
    for head in range(LANES // width):
        only = lane == head
        pick = (lambda a: a) if width == LANES else (lambda a: jnp.where(only, a, 0.0))
        pairs = mm_nt(pick(queries), sources)
        remove_remove = jnp.where(strict, pairs[:T, :T], 0.0)
        remove_key = jnp.where(strict, pairs[:T, T:], 0.0)
        read_remove = jnp.where(inclusive, pairs[T:, :T], 0.0)
        read_key = jnp.where(inclusive, pairs[T:, T:], 0.0)
        inverse = unit_inverse(remove_remove, rows, cols)
        value = pick(v)
        carried = mm(inverse, mm(remove_key, value))
        start = mm(inverse, pick(start_target))
        local_out = local_out + mm(read_remove, carried) + mm(read_key, value)
        start_read = start_read + mm(read_remove, start)
        head_right = pick(right_tail)
        transit = transit + mm(start.T, head_right)
        added = added + mm(carried.T, head_right) + mm(value.T, pick(key_tail))
    return local_out, start_read, transit, added


def finish_unit(width, read, q, k, v, gain, own, gate):
    ones = same_head(width)
    mean = mm(read, ones) / width
    centered = read - mean
    variance = mm(centered * centered, ones) / width
    normed = centered * lax.rsqrt(variance + head_epsilon) * gain
    diagonal = mm(q * k * own, ones) * v
    return ((normed + diagonal) * gate).astype(jnp.bfloat16)


def attention_kernel(
    n_sp, widths, q_ref, k_ref, v_ref, f_ref, a_ref, e_ref, g_ref, gain_ref, own_ref,
    first_ref, second_ref, mixed_ref, first_out, second_out,
    local_ref, read_ref, mine, got, send_sem, recv_sem,
    up_sem, down_sem, along_sem, side_sem, side_recv, keep_sem,
):
    me = lax.axis_index("sp")
    tp = lax.axis_index("tp")

    barrier = pltpu.get_barrier_semaphore()

    @pl.loop(1, n_sp)
    def _(d):
        pl.semaphore_signal(
            barrier, inc=1, device_id=(lax.rem(me + d, n_sp), tp), device_id_type=MESH
        )

    pl.semaphore_wait(barrier, n_sp - 1)

    line, side = me // 2, me % 2
    length = n_sp // 2
    weights = ((first_ref, first_out), (second_ref, second_out))

    def pass_on(w, block, to, source, sem, landed):
        return pltpu.make_async_remote_copy(
            src_ref=source, dst_ref=weights[w][1].at[block], send_sem=sem, recv_sem=landed,
            device_id=(to, tp), device_id_type=MESH,
        )

    def to_line(w, at, to, source, sem):
        return pass_on(w, at * 2 + side, to * 2 + side, source, sem.at[w, at], along_sem.at[w, at])

    def to_side(w, at, source):
        return pass_on(
            w, at * 2 + side, line * 2 + 1 - side, source, side_sem.at[w, at], side_recv.at[w, at]
        )

    def spread(w, at, source, upward, downward):
        if upward:

            @pl.when(line + 1 < length)
            def _():
                to_line(w, at, line + 1, source, up_sem).start()

        if downward:

            @pl.when(line >= 1)
            def _():
                to_line(w, at, line - 1, source, down_sem).start()

        to_side(w, at, source).start()

    def relay(i):
        for w in range(2):
            below, above = line - i, line + i

            @pl.when(below >= 0)
            def _():
                source = weights[w][1].at[below * 2 + side]
                to_line(w, below, line, source, up_sem).wait_recv()
                spread(w, below, source, True, False)

            @pl.when(above < length)
            def _():
                source = weights[w][1].at[above * 2 + side]
                to_line(w, above, line, source, down_sem).wait_recv()
                spread(w, above, source, False, True)

    for w in range(2):
        spread(w, line, weights[w][0], True, True)
    keeps = [
        pltpu.make_async_copy(weights[w][0], weights[w][1].at[me], keep_sem.at[w])
        for w in range(2)
    ]
    for keep in keeps:
        keep.start()

    per_group = q_ref.shape[2] // LANES

    def load(ref, g, c):
        return ref[g, :, c * LANES : (c + 1) * LANES].astype(jnp.float32)

    def copy(u, d, to):
        return pltpu.make_async_remote_copy(
            src_ref=mine.at[u],
            dst_ref=got.at[d, u],
            send_sem=send_sem.at[u, d],
            recv_sem=recv_sem.at[u, d],
            device_id=(to, tp),
            device_id_type=MESH,
        )

    units = [(g, c) for g in range(2) for c in range(per_group)]
    for u, (g, c) in enumerate(units):
        local_out, start_read, transit, added = local_unit(
            widths[g], *(load(r, g, c) for r in (q_ref, k_ref, v_ref, f_ref, a_ref, e_ref))
        )
        local_ref[u] = local_out
        read_ref[u] = start_read
        mine[u, 0] = transit.astype(jnp.bfloat16)
        mine[u, 1] = added.astype(jnp.bfloat16)

        @pl.loop(1, n_sp)
        def _(d):
            @pl.when(me + d < n_sp)
            def _():
                copy(u, d, me + d).start()

        if u == 1 and length > 1:
            relay(1)
        if u == 3 and length > 2:
            relay(2)

    for u in range(len(units)):

        @pl.loop(1, n_sp)
        def _(d):
            @pl.when(me - d >= 0)
            def _():
                copy(u, d, me).wait_recv()

    def fold(step, states):
        d = me - step
        return tuple(
            mm(s, got[d, u, 0]) + got[d, u, 1].astype(jnp.float32)
            for u, s in enumerate(states)
        )

    states = lax.fori_loop(
        0, me, fold, tuple(jnp.zeros((LANES, LANES), jnp.float32) for _ in units)
    )
    for u, (g, c) in enumerate(units):
        lanes = slice(c * LANES, (c + 1) * LANES)
        read = local_ref[u] + mm_nt(read_ref[u], states[u])
        mixed = finish_unit(
            widths[g], read, load(q_ref, g, c), load(k_ref, g, c), load(v_ref, g, c),
            gain_ref[g : g + 1, lanes], own_ref[g : g + 1, lanes], load(g_ref, g, c),
        )
        mixed_ref[:, u * LANES : (u + 1) * LANES] = mixed

    for i in range(3, length):
        relay(i)

    for keep in keeps:
        keep.wait()

    @pl.loop(0, length)
    def _(at):
        for w in range(2):
            source = weights[w][0]
            to_side(w, at, source).wait()

            @pl.when((at <= line) & (line + 1 < length))
            def _():
                to_line(w, at, line + 1, source, up_sem).wait_send()

            @pl.when((at >= line) & (line >= 1))
            def _():
                to_line(w, at, line - 1, source, down_sem).wait_send()

    for u in range(len(units)):

        @pl.loop(1, n_sp)
        def _(d):
            @pl.when(me + d < n_sp)
            def _():
                copy(u, d, me + d).wait_send()


def attention(n_sp, q, k, v, f, a, e, g, gain, own, first, second):
    T, channels = q.shape[1], q.shape[2]
    units = 2 * channels // LANES
    vmem = pl.BlockSpec(memory_space=pltpu.VMEM)
    return pl.pallas_call(
        functools.partial(attention_kernel, n_sp, (DS, DL)),
        out_shape=[
            jax.ShapeDtypeStruct((T, 2 * channels), jnp.bfloat16),
            jax.ShapeDtypeStruct((n_sp,) + first.shape, first.dtype),
            jax.ShapeDtypeStruct((n_sp,) + second.shape, second.dtype),
        ],
        in_specs=[vmem] * 11,
        out_specs=[vmem, pl.BlockSpec(memory_space=pl.ANY), pl.BlockSpec(memory_space=pl.ANY)],
        scratch_shapes=[
            pltpu.VMEM((units, T, LANES), jnp.float32),
            pltpu.VMEM((units, T, LANES), jnp.float32),
            pltpu.VMEM((units, 2, LANES, LANES), jnp.bfloat16),
            pltpu.VMEM((n_sp, units, 2, LANES, LANES), jnp.bfloat16),
            pltpu.SemaphoreType.DMA((units, n_sp)),
            pltpu.SemaphoreType.DMA((units, n_sp)),
        ]
        + [pltpu.SemaphoreType.DMA((2, n_sp // 2))] * 5
        + [pltpu.SemaphoreType.DMA((2,))],
        compiler_params=pltpu.CompilerParams(
            collective_id=0, has_side_effects=True, vmem_limit_bytes=60 * 2**20
        ),
        cost_estimate=pl.CostEstimate(
            flops=15 * 10**10, bytes_accessed=2**28, transcendentals=0
        ),
        name="attention",
    )(q, k, v, f, a, e, g, gain, own, first, second)


def on_device(
    stratum_source_matrix,
    acceptance_query,
    cluster_lookup_matrix,
    cluster_payload_matrix,
    fading_logit,
    adaptation_speed_logit,
    additional_fading_exponent,
    result_switch_pair,
    attender_scaling_factor,
    present_item_factor,
    final_mapping_matrix,
    perceptron_scaling_factor,
    switching_matrix,
    widening_matrix,
    shrinking_matrix,
):
    down_whole = lax.all_gather(shrinking_matrix, "sp", axis=1, tiled=True)
    mixed, gate_whole, up_whole = attention(
        lax.axis_size("sp"),
        acceptance_query,
        cluster_lookup_matrix,
        cluster_payload_matrix,
        fading_logit,
        adaptation_speed_logit,
        additional_fading_exponent,
        result_switch_pair,
        attender_scaling_factor,
        present_item_factor,
        switching_matrix,
        widening_matrix,
    )
    gate_whole = gate_whole.reshape(-1, gate_whole.shape[2])
    up_whole = up_whole.reshape(-1, up_whole.shape[2])
    partial_value = jnp.dot(
        mixed,
        final_mapping_matrix.reshape(-1, final_mapping_matrix.shape[2]),
        preferred_element_type=jnp.float32,
    )
    columns = perceptron_scaling_factor.shape[0] // lax.axis_size("tp")
    own_start = lax.axis_index("tp") * columns
    residual_float = stratum_source_matrix.astype(jnp.float32)
    branch = lax.psum_scatter(
        partial_value.astype(jnp.bfloat16), "tp", scatter_dimension=1, tiled=True
    ).astype(jnp.float32)
    own_residual = lax.dynamic_slice_in_dim(residual_float, own_start, columns, 1)
    own_state = (own_residual + branch).astype(jnp.bfloat16).astype(jnp.float32)
    square_total = lax.psum(jnp.sum(own_state * own_state, axis=1), "tp")
    own_gain = lax.dynamic_slice_in_dim(perceptron_scaling_factor, own_start, columns, 0)
    scaled = (
        own_state
        * lax.rsqrt(square_total / perceptron_scaling_factor.shape[0] + norm_epsilon)[:, None]
        * own_gain
    )
    normed = lax.all_gather(scaled.astype(jnp.bfloat16), "tp", axis=1, tiled=True)
    gate_pre = jnp.dot(normed, gate_whole, preferred_element_type=jnp.float32)
    up_pre = jnp.dot(normed, up_whole, preferred_element_type=jnp.float32)
    activated = (jax.nn.silu(gate_pre) * up_pre).astype(jnp.bfloat16)
    down_terms = jnp.dot(
        activated,
        down_whole,
        preferred_element_type=jnp.float32,
    )
    mixer = lax.psum_scatter(
        down_terms.astype(jnp.bfloat16), "tp", scatter_dimension=1, tiled=True
    ).astype(jnp.float32)
    return (own_state + mixer).astype(jnp.bfloat16)


def solution(mesh):
    tokens = P(None, "sp", "tp")
    in_specs = (
        P("sp", None), tokens, tokens, tokens, tokens, tokens, tokens, tokens,
        P(None, "tp"), P(None, "tp"), P(None, "tp", None), P(),
        P("sp", "tp"), P("sp", "tp"), P("tp", "sp"),
    )
    return jax.shard_map(
        on_device, mesh=mesh, in_specs=in_specs, out_specs=P("sp", "tp"), check_vma=False
    )
```
